32 devices in a mesh: fs: 16 (over z, y, x), tp: 2 (over core).
Axes of the slice: x: 2, y: 2, z: 4, core: 2. Of those that a mesh axis runs over, the one named last changes fastest.
Arguments:
- tokens: bfloat16 [4096, 2048], P('fs', 'tp'), may hold values from -6 to 6
- mixer_norm_gain: bfloat16 [2048], replicated, may hold values from 0.099609375 to 1.8984375
- recurrence_branch_weight: bfloat16 [2048, 1024], P('fs', 'tp'), may hold values from -0.125 to 0.125
- output_gate_projection: bfloat16 [2048, 1024], P('fs', 'tp'), may hold values from -0.125 to 0.125
- recurrence_conv_taps: bfloat16 [4, 1024], P(None, 'tp'), may hold values from -3 to 3
- recurrence_gate_map: bfloat16 [16, 64, 64], P('tp'), may hold values from -0.75 to 0.75
- input_gate_map: bfloat16 [16, 64, 64], P('tp'), may hold values from -0.75 to 0.75
- channel_decay_rate: float32 [1024], P('tp'), may hold values from 0.001 to 0.03
- position_log_decay: float32 [4096, 1024], P('fs', 'tp'), may hold values from -0.69 to 0
- mixer_output_weight: bfloat16 [1024, 2048], P('tp', 'fs'), may hold values from -0.75 to 0.75
- feedforward_norm_gain: bfloat16 [2048], replicated, may hold values from 0.099609375 to 1.8984375
- gate_up_weight: bfloat16 [2048, 5632], P('fs', 'tp'), may hold values from -0.125 to 0.125
- value_up_weight: bfloat16 [2048, 5632], P('fs', 'tp'), may hold values from -0.125 to 0.125
- gate_conv_taps: bfloat16 [3, 5632], P(None, 'tp'), may hold values from -3 to 3
- value_conv_taps: bfloat16 [3, 5632], P(None, 'tp'), may hold values from -3 to 3
- down_projection_weight: bfloat16 [5632, 2048], P('tp', 'fs'), may hold values from -0.15625 to 0.15625
Outputs:
- result: bfloat16 [4096, 2048], P('fs', 'tp')
The draws below stay inside these ranges and needn't reach their ends.
All inputs are finite; a program needn't handle non-finite values.
Results may differ from the reference program's by a relative error of at most 0.024.
Values may be sent and summed in bfloat16 or wider, within the bound.
No kernel may reach another device: no remote copies, remote signals or barrier semaphores. Data moves between devices by JAX's collectives and lax.ppermute only.
A program may use at most 128 MiB of HBM per device.

```python
import math
import jax
import jax.numpy as jnp
from jax import lax

D = 2048
HEADS = 16
HEAD_DIM = 64
W = 1024
FF = 5632
SEQ_LEN = 64
TOKENS = 4096
N_TP = 2


def draw_channel_decay_rate(key, part):
    base = jax.random.fold_in(key, 17)
    key_pick, key_slow, key_fast = jax.random.split(base, 3)
    limit = 5
    picked = jax.random.randint(key_pick, (W,), 0, 10) < limit
    slow_rate = jnp.exp(jax.random.uniform(key_slow, (W,), jnp.float32, math.log(0.001), math.log(0.004)))
    fast_rate = jnp.exp(jax.random.uniform(key_fast, (W,), jnp.float32, math.log(0.012), math.log(0.03)))
    return jnp.where(picked, slow_rate, fast_rate).astype(jnp.float32)


def draw_position_log_decay(key, part):
    base = jax.random.fold_in(key, 29)
    key_marks, key_depth = jax.random.split(base, 2)
    marks = (jax.random.randint(key_marks, (TOKENS, 1), 0, 32) == 0).astype(jnp.float32)
    depth = jax.random.uniform(key_depth, (TOKENS, W), jnp.float32, 0.22, 0.69)
    return (-marks * depth).astype(jnp.float32)


def steps_of(rng, extent, pieces, low, top_value):
    level, own = 1.0, jax.random.fold_in(rng, 6)
    for position, parts in pieces:
        steps = jnp.exp(jax.random.uniform(jax.random.fold_in(own, position), (parts,), jnp.float32, low / len(pieces), top_value / len(pieces)))
        level = level * jnp.repeat(steps, extent[position] // parts).reshape([-1 if axis == position else 1 for axis in range(len(extent))])
    return level


def normal_values(stream_key, extent, scale, most, shards=(), dtype=jnp.bfloat16):
    drawn = jax.random.normal(stream_key, extent, jnp.float32) * scale
    if len(shards) > 0:
        drawn = steps_of(stream_key, extent, shards, -0.22, 0.18) * drawn
    return jnp.clip(drawn, min=-most, max=most).astype(dtype)


def setup_inputs(seed: int = 0) -> dict:
    key_list = jax.random.split(jax.random.key(seed), 17)
    tokens = normal_values(key_list[0], (TOKENS, D), 1.0, 6.0, ((0, 16), (1, 2)))
    mixer_norm_gain = jnp.clip(1.0 + 0.18 * jax.random.normal(key_list[1], (D,), jnp.float32), 0.099609375, 1.8984375).astype(jnp.bfloat16)
    recurrence_branch_weight = normal_values(key_list[2], (D, W), D ** -0.5, 0.125, ((0, 16), (1, 2)))
    output_gate_projection = normal_values(key_list[3], (D, W), D ** -0.5, 0.125, ((0, 16), (1, 2)))
    recurrence_conv_taps = normal_values(key_list[4], (4, W), 0.5, 3.0, ((1, 2),))
    recurrence_gate_map = normal_values(key_list[5], (HEADS, HEAD_DIM, HEAD_DIM), HEAD_DIM ** -0.5, 0.75, ((0, 2),))
    input_gate_map = normal_values(key_list[6], (HEADS, HEAD_DIM, HEAD_DIM), HEAD_DIM ** -0.5, 0.75, ((0, 2),))
    channel_decay_rate = draw_channel_decay_rate(jax.random.fold_in(key_list[16], 71), 0)
    position_log_decay = draw_position_log_decay(jax.random.fold_in(key_list[16], 71), 0)
    mixer_output_weight = normal_values(key_list[9], (W, D), (W // 16) ** -0.5, 0.75, ((0, 2), (1, 16)))
    feedforward_norm_gain = jnp.clip(1.0 + 0.18 * jax.random.normal(key_list[10], (D,), jnp.float32), 0.099609375, 1.8984375).astype(jnp.bfloat16)
    gate_up_weight = normal_values(key_list[11], (D, FF), D ** -0.5, 0.125, ((0, 16), (1, 2)))
    value_up_weight = normal_values(key_list[12], (D, FF), D ** -0.5, 0.125, ((0, 16), (1, 2)))
    gate_conv_taps = normal_values(key_list[13], (3, FF), 0.6, 3.0, ((1, 2),))
    value_conv_taps = normal_values(key_list[14], (3, FF), 0.6, 3.0, ((1, 2),))
    down_projection_weight = normal_values(key_list[15], (FF, D), (FF // 4) ** -0.5, 0.15625, ((0, 2), (1, 16)))
    return {"tokens": tokens, "mixer_norm_gain": mixer_norm_gain, "recurrence_branch_weight": recurrence_branch_weight, "output_gate_projection": output_gate_projection, "recurrence_conv_taps": recurrence_conv_taps, "recurrence_gate_map": recurrence_gate_map, "input_gate_map": input_gate_map, "channel_decay_rate": channel_decay_rate, "position_log_decay": position_log_decay, "mixer_output_weight": mixer_output_weight, "feedforward_norm_gain": feedforward_norm_gain, "gate_up_weight": gate_up_weight, "value_up_weight": value_up_weight, "gate_conv_taps": gate_conv_taps, "value_conv_taps": value_conv_taps, "down_projection_weight": down_projection_weight}


EPS = 1e-06
DECAY_RATE_GAIN = 8.0

def rms_normed(values, gain):
    wide = values.astype(jnp.float32)
    factor = lax.rsqrt(lax.optimization_barrier(jnp.mean(wide * wide, axis=-1, keepdims=True)) + EPS)
    return (wide * factor * gain.astype(jnp.float32)).astype(jnp.bfloat16)

def causal_conv(values, kernel):
    width = kernel.shape[0]
    row_count, channels = values.shape
    grouped = values.astype(jnp.float32).reshape(row_count // SEQ_LEN, SEQ_LEN, channels)
    padded = jnp.pad(grouped, ((0, 0), (width - 1, 0), (0, 0)))
    summed = padded[:, 0:SEQ_LEN] * kernel[0].astype(jnp.float32)
    for offset in range(1, width):
        summed = summed + padded[:, offset:offset + SEQ_LEN] * kernel[offset].astype(jnp.float32)
    return summed.reshape(row_count, channels)

def combine(left, right):
    first_a, first_b = left
    second_a, second_b = right
    return (first_a * second_a, second_a * first_b + second_b)

def block_sums(left, weight, blocks):
    width = left.shape[1] // blocks
    summed = jnp.zeros((left.shape[0], weight.shape[1]), jnp.float32)
    for index in range(blocks):
        partial_sum = jnp.dot(left[:, index * width:(index + 1) * width], weight[index * width:(index + 1) * width], preferred_element_type=jnp.float32)
        summed = summed + partial_sum.astype(jnp.bfloat16).astype(jnp.float32)
    return summed

def reference(tokens, mixer_norm_gain, recurrence_branch_weight, output_gate_projection, recurrence_conv_taps, recurrence_gate_map, input_gate_map, channel_decay_rate, position_log_decay, mixer_output_weight, feedforward_norm_gain, gate_up_weight, value_up_weight, gate_conv_taps, value_conv_taps, down_projection_weight):
    row_count = tokens.shape[0]
    normed = rms_normed(tokens, mixer_norm_gain)
    branch = jnp.dot(normed, recurrence_branch_weight, preferred_element_type=jnp.float32).astype(jnp.bfloat16)
    outgate = jnp.dot(normed, output_gate_projection, preferred_element_type=jnp.float32).astype(jnp.bfloat16)
    conv = causal_conv(branch, recurrence_conv_taps).astype(jnp.bfloat16)
    grouped = conv.astype(jnp.float32).reshape(row_count, HEADS, HEAD_DIM)
    recurrence_scan = jax.nn.sigmoid(jnp.einsum('rhi,hij->rhj', grouped, recurrence_gate_map.astype(jnp.float32)).reshape(row_count, W))
    inner = jax.nn.sigmoid(jnp.einsum('rhi,hij->rhj', grouped, input_gate_map.astype(jnp.float32)).reshape(row_count, W))
    log_alpha = -DECAY_RATE_GAIN * recurrence_scan * channel_decay_rate[None, :] + position_log_decay
    drive = jnp.sqrt(-jnp.expm1(2.0 * log_alpha)) * inner * conv.astype(jnp.float32)
    shape3 = (row_count // SEQ_LEN, SEQ_LEN, W)
    unused, state = lax.associative_scan(combine, (jnp.exp(log_alpha).reshape(shape3), drive.reshape(shape3)), axis=1)
    state = state.reshape(row_count, W)
    mixed = (state * jax.nn.gelu(outgate.astype(jnp.float32))).astype(jnp.bfloat16)
    after = (tokens.astype(jnp.float32) + block_sums(mixed, mixer_output_weight, N_TP)).astype(jnp.bfloat16)
    normed2 = rms_normed(after, feedforward_norm_gain)
    gate_half = jnp.dot(normed2, gate_up_weight, preferred_element_type=jnp.float32).astype(jnp.bfloat16)
    value_half = jnp.dot(normed2, value_up_weight, preferred_element_type=jnp.float32).astype(jnp.bfloat16)
    hidden = (jax.nn.silu(causal_conv(gate_half, gate_conv_taps)) * causal_conv(value_half, value_conv_taps)).astype(jnp.bfloat16)
    return (after.astype(jnp.float32) + block_sums(hidden, down_projection_weight, N_TP)).astype(jnp.bfloat16)
```

```python
import functools

import jax
import jax.numpy as jnp
from jax import lax
from jax.sharding import Mesh
from jax.sharding import PartitionSpec as P

SEQ_LEN = 64


EPS = 1e-06
DECAY_RATE_GAIN = 8.0


def rms_normed(values, gain):
    wide = values.astype(jnp.float32)
    factor = lax.rsqrt(jnp.mean(wide * wide, axis=-1, keepdims=True) + EPS)
    return (wide * factor * gain.astype(jnp.float32)).astype(jnp.bfloat16)


def causal_conv(values, kernel):
    width = kernel.shape[0]
    row_count, channels = values.shape
    grouped = values.astype(jnp.float32).reshape(row_count // SEQ_LEN, SEQ_LEN, channels)
    padded = jnp.pad(grouped, ((0, 0), (width - 1, 0), (0, 0)))
    summed = padded[:, 0:SEQ_LEN] * kernel[0].astype(jnp.float32)
    for offset in range(1, width):
        summed = summed + padded[:, offset : offset + SEQ_LEN] * kernel[offset].astype(jnp.float32)
    return summed.reshape(row_count, channels)


def combine(left, right):
    first_a, first_b = left
    second_a, second_b = right
    return (first_a * second_a, second_a * first_b + second_b)


def pair_folder(normed, pieces):
    return (
        jnp.dot(normed, pieces[0], preferred_element_type=jnp.float32),
        jnp.dot(normed, pieces[1], preferred_element_type=jnp.float32),
    )


def gathered_layer(
    tokens,
    mixer_norm_gain,
    recurrence_branch_weight,
    output_gate_projection,
    recurrence_conv_taps,
    recurrence_gate_map,
    input_gate_map,
    channel_decay_rate,
    position_log_decay,
    mixer_output_weight,
    feedforward_norm_gain,
    gate_up_weight,
    value_up_weight,
    gate_conv_taps,
    value_conv_taps,
    down_projection_weight,
):
    row_count = tokens.shape[0]
    local_width = recurrence_branch_weight.shape[1]
    local_heads = recurrence_gate_map.shape[0]
    head_size = recurrence_gate_map.shape[1]
    whole_rows = lax.all_gather(tokens, "tp", axis=1, tiled=True)
    normed = rms_normed(whole_rows, mixer_norm_gain)
    branch_sum, outgate_sum = pair_folder(
        normed,
        (
            lax.all_gather(recurrence_branch_weight, "fs", axis=0, tiled=True),
            lax.all_gather(output_gate_projection, "fs", axis=0, tiled=True),
        ),
    )
    branch = branch_sum.astype(jnp.bfloat16)
    outgate = outgate_sum.astype(jnp.bfloat16)
    conv = causal_conv(branch, recurrence_conv_taps).astype(jnp.bfloat16)
    grouped = conv.reshape(row_count, local_heads, head_size)
    recurrence_scan = jax.nn.sigmoid(
        jnp.einsum(
            "rhi,hij->rhj", grouped, recurrence_gate_map, preferred_element_type=jnp.float32
        ).reshape(row_count, local_width)
    )
    inner = jax.nn.sigmoid(
        jnp.einsum(
            "rhi,hij->rhj", grouped, input_gate_map, preferred_element_type=jnp.float32
        ).reshape(row_count, local_width)
    )
    log_alpha = (
        -DECAY_RATE_GAIN * recurrence_scan * channel_decay_rate[None, :] + position_log_decay
    )
    drive = jnp.sqrt(-jnp.expm1(2.0 * log_alpha)) * inner * conv.astype(jnp.float32)
    shape3 = (row_count // SEQ_LEN, SEQ_LEN, local_width)
    unused, state = lax.associative_scan(
        combine, (jnp.exp(log_alpha).reshape(shape3), drive.reshape(shape3)), axis=1
    )
    state = state.reshape(row_count, local_width)
    mixed = (state * jax.nn.gelu(outgate.astype(jnp.float32))).astype(jnp.bfloat16)
    mixer_terms = jnp.dot(
        mixed,
        lax.all_gather(mixer_output_weight, "fs", axis=1, tiled=True),
        preferred_element_type=jnp.float32,
    )
    mixer_terms = mixer_terms.astype(jnp.bfloat16).astype(jnp.float32)
    mixer_whole = lax.psum(mixer_terms.astype(jnp.bfloat16), "tp").astype(jnp.float32)
    whole_after = (whole_rows.astype(jnp.float32) + mixer_whole).astype(jnp.bfloat16)
    normed2 = rms_normed(whole_after, feedforward_norm_gain)
    gate_whole, value_whole = (
        lax.all_gather(gate_up_weight, "fs", axis=0, tiled=True),
        lax.all_gather(value_up_weight, "fs", axis=0, tiled=True),
    )
    gate_sum = jnp.dot(normed2, gate_whole, preferred_element_type=jnp.float32)
    value_sum = jnp.dot(normed2, value_whole, preferred_element_type=jnp.float32)
    gate_half = gate_sum.astype(jnp.bfloat16)
    value_half = value_sum.astype(jnp.bfloat16)
    hidden = (
        jax.nn.silu(causal_conv(gate_half, gate_conv_taps))
        * causal_conv(value_half, value_conv_taps)
    ).astype(jnp.bfloat16)
    channel_terms = jnp.dot(
        hidden,
        lax.all_gather(down_projection_weight, "fs", axis=1, tiled=True),
        preferred_element_type=jnp.float32,
    )
    channel_terms = channel_terms.astype(jnp.bfloat16).astype(jnp.float32)
    channel_share = lax.psum_scatter(
        channel_terms.astype(jnp.bfloat16), "tp", scatter_dimension=1, tiled=True
    ).astype(jnp.float32)
    share_width = channel_share.shape[1]
    residual_share = lax.dynamic_slice_in_dim(
        whole_after, lax.axis_index("tp") * share_width, share_width, 1
    )
    return (residual_share.astype(jnp.float32) + channel_share).astype(jnp.bfloat16)


def exchange(values, axis, pairs):
    return lax.ppermute(values, axis, pairs)


def shifted(values, axis, size, step):
    return lax.ppermute(values, axis, [(k, (k + step) % size) for k in range(size)])


def square_gather(values):
    half = values.shape[0] // 2
    across = [(k, k ^ 1) for k in range(4)]
    along = [(k, k ^ 2) for k in range(4)]
    first = lax.ppermute(values, "p", across)
    second = lax.ppermute(values, "p", along)
    top = lax.ppermute(second[:half], "p", across)
    bottom = lax.ppermute(first[half:], "p", along)
    return [(0, 0, values), (1, 0, first), (2, 0, second), (3, 0, top), (3, half, bottom)]


def split_layer(
    depth,
    tokens,
    mixer_norm_gain,
    recurrence_branch_weight,
    output_gate_projection,
    recurrence_conv_taps,
    recurrence_gate_map,
    input_gate_map,
    channel_decay_rate,
    position_log_decay,
    mixer_output_weight,
    feedforward_norm_gain,
    gate_up_weight,
    value_up_weight,
    gate_conv_taps,
    value_conv_taps,
    down_projection_weight,
):
    row_count, share_width = tokens.shape
    width = 2 * share_width
    local_width = recurrence_branch_weight.shape[1]
    local_heads = recurrence_gate_map.shape[0]
    head_size = recurrence_gate_map.shape[1]
    chunk = recurrence_branch_weight.shape[0]
    units = gate_up_weight.shape[1] // depth
    z, p, c = lax.axis_index("z"), lax.axis_index("p"), lax.axis_index("c")
    swap = [(0, 1), (1, 0)]

    def both_halves(mine):
        other = lax.ppermute(mine, "c", swap)
        return jnp.where(
            c == 0,
            jnp.concatenate([mine, other], axis=1),
            jnp.concatenate([other, mine], axis=1),
        )

    whole_rows = both_halves(tokens)

    rows_out = local_width // chunk
    mixer_piece = jnp.concatenate(
        [recurrence_branch_weight, output_gate_projection]
        + [mixer_output_weight[chunk * r : chunk * (r + 1)] for r in range(rows_out)],
        axis=1,
    )
    mixer_pieces = [mixer_piece] + [shifted(mixer_piece, "z", depth, s) for s in range(1, depth)]

    up_blocks = jnp.stack(
        [
            jnp.concatenate(
                [gate_up_weight[:, units * k : units * (k + 1)], value_up_weight[:, units * k : units * (k + 1)]],
                axis=1,
            )
            for k in range(depth)
        ]
    )
    down_blocks = down_projection_weight.reshape(depth, units, chunk)
    up_pieces, down_pieces = [], []
    for s in range(depth):
        up = lax.dynamic_index_in_dim(up_blocks, (z + s) % depth, 0, False)
        down = lax.dynamic_index_in_dim(down_blocks, (z + s) % depth, 0, False)
        up_pieces.append(up if s == 0 else shifted(up, "z", depth, s))
        down_pieces.append(down if s == 0 else shifted(down, "z", depth, s))

    mixer_in = jnp.zeros((width, 2 * local_width), jnp.bfloat16)
    mixer_out = jnp.zeros((local_width, width), jnp.bfloat16)
    for s in range(depth):
        for place, row, part in square_gather(mixer_pieces[s]):
            at = (((z - s) % depth) * 4 + (p ^ place)) * chunk
            mixer_in = lax.dynamic_update_slice(mixer_in, part[:, : 2 * local_width], (at + row, 0))
            for r in range(rows_out):
                lane = 2 * local_width + chunk * r
                mixer_out = lax.dynamic_update_slice(
                    mixer_out, part[:, lane : lane + chunk], (chunk * r + row, at)
                )

    normed = rms_normed(whole_rows, mixer_norm_gain)
    both = jnp.dot(normed, mixer_in, preferred_element_type=jnp.float32).astype(jnp.bfloat16)
    branch, outgate = both[:, :local_width], both[:, local_width:]
    conv = causal_conv(branch, recurrence_conv_taps).astype(jnp.bfloat16)
    grouped = conv.reshape(row_count, local_heads, head_size)
    recurrence_scan = jax.nn.sigmoid(
        jnp.einsum(
            "rhi,hij->rhj", grouped, recurrence_gate_map, preferred_element_type=jnp.float32
        ).reshape(row_count, local_width)
    )
    inner = jax.nn.sigmoid(
        jnp.einsum(
            "rhi,hij->rhj", grouped, input_gate_map, preferred_element_type=jnp.float32
        ).reshape(row_count, local_width)
    )
    log_alpha = (
        -DECAY_RATE_GAIN * recurrence_scan * channel_decay_rate[None, :] + position_log_decay
    )
    drive = jnp.sqrt(-jnp.expm1(2.0 * log_alpha)) * inner * conv.astype(jnp.float32)
    shape3 = (row_count // SEQ_LEN, SEQ_LEN, local_width)
    unused, state = lax.associative_scan(
        combine, (jnp.exp(log_alpha).reshape(shape3), drive.reshape(shape3)), axis=1
    )
    state = state.reshape(row_count, local_width)
    mixed = (state * jax.nn.gelu(outgate.astype(jnp.float32))).astype(jnp.bfloat16)
    mine = jnp.dot(mixed, mixer_out, preferred_element_type=jnp.float32).astype(jnp.bfloat16)
    theirs = lax.ppermute(mine, "c", swap)
    whole_after = (
        whole_rows.astype(jnp.float32) + (mine.astype(jnp.float32) + theirs.astype(jnp.float32))
    ).astype(jnp.bfloat16)
    normed2 = rms_normed(whole_after, feedforward_norm_gain)
    own_half = lax.dynamic_slice_in_dim(normed2, c * share_width, share_width, 1)
    rows_in = [normed2] + [both_halves(shifted(own_half, "z", depth, s)) for s in range(1, depth)]

    up_weight = jnp.zeros((width, 2 * units), jnp.bfloat16)
    down_weight = jnp.zeros((units, width), jnp.bfloat16)
    for s in range(depth):
        for place, row, part in square_gather(up_pieces[s]):
            at = (((z - s) % depth) * 4 + (p ^ place)) * chunk
            up_weight = lax.dynamic_update_slice(up_weight, part, (at + row, 0))
    for s in range(depth):
        for place, row, part in square_gather(down_pieces[s]):
            at = (((z - s) % depth) * 4 + (p ^ place)) * chunk
            down_weight = lax.dynamic_update_slice(down_weight, part, (row, at))

    gate_taps = lax.dynamic_slice_in_dim(gate_conv_taps, z * units, units, 1)
    value_taps = lax.dynamic_slice_in_dim(value_conv_taps, z * units, units, 1)

    total = None
    for s in range(depth):
        sums = jnp.dot(rows_in[s], up_weight, preferred_element_type=jnp.float32).astype(jnp.bfloat16)
        hidden = (
            jax.nn.silu(causal_conv(sums[:, :units], gate_taps)) * causal_conv(sums[:, units:], value_taps)
        ).astype(jnp.bfloat16)
        product = jnp.dot(hidden, down_weight, preferred_element_type=jnp.float32).astype(jnp.bfloat16)
        kept = lax.dynamic_slice_in_dim(product, c * share_width, share_width, 1)
        given = lax.dynamic_slice_in_dim(product, (1 - c) * share_width, share_width, 1)
        taken = lax.ppermute(given, "c", swap)
        joined = kept.astype(jnp.float32) + taken.astype(jnp.float32)
        if s > 0:
            joined = shifted(joined.astype(jnp.bfloat16), "z", depth, depth - s).astype(jnp.float32)
        total = joined if total is None else total + joined
    residual = lax.dynamic_slice_in_dim(whole_after, c * share_width, share_width, 1)
    return (residual.astype(jnp.float32) + total).astype(jnp.bfloat16)


def solution(mesh):
    placed = (
        P("fs", "tp"),
        P(),
        P("fs", "tp"),
        P("fs", "tp"),
        P(None, "tp"),
        P("tp", None, None),
        P("tp", None, None),
        P("tp"),
        P("fs", "tp"),
        P("tp", "fs"),
        P(),
        P("fs", "tp"),
        P("fs", "tp"),
        P(None, "tp"),
        P(None, "tp"),
        P("tp", "fs"),
    )
    shards, cores = mesh.shape["fs"], mesh.shape["tp"]
    if cores != 2 or shards % 4 != 0 or shards // 4 > 4:
        return jax.shard_map(
            gathered_layer, mesh=mesh, in_specs=placed, out_specs=P("fs", "tp"), check_vma=False
        )
    depth = shards // 4
    finer = Mesh(mesh.devices.reshape(depth, 4, cores), ("z", "p", "c"))
    names = {"fs": ("z", "p"), "tp": "c", None: None}
    split = tuple(P(*[names[name] for name in spec]) for spec in placed)
    return jax.shard_map(
        functools.partial(split_layer, depth),
        mesh=finer,
        in_specs=split,
        out_specs=P(("z", "p"), "c"),
        check_vma=False,
    )
```

```python
import functools

import jax
import jax.numpy as jnp
from jax import lax
from jax.experimental import pallas as pl
from jax.experimental.pallas import tpu as pltpu
from jax.sharding import Mesh
from jax.sharding import PartitionSpec as P

SEQ_LEN = 64


EPS = 1e-06
DECAY_RATE_GAIN = 8.0


def rms_normed(values, gain):
    wide = values.astype(jnp.float32)
    factor = lax.rsqrt(jnp.mean(wide * wide, axis=-1, keepdims=True) + EPS)
    return (wide * factor * gain.astype(jnp.float32)).astype(jnp.bfloat16)


def causal_conv(values, kernel):
    width = kernel.shape[0]
    row_count, channels = values.shape
    grouped = values.astype(jnp.float32).reshape(row_count // SEQ_LEN, SEQ_LEN, channels)
    padded = jnp.pad(grouped, ((0, 0), (width - 1, 0), (0, 0)))
    summed = padded[:, 0:SEQ_LEN] * kernel[0].astype(jnp.float32)
    for offset in range(1, width):
        summed = summed + padded[:, offset : offset + SEQ_LEN] * kernel[offset].astype(jnp.float32)
    return summed.reshape(row_count, channels)


def combine(left, right):
    first_a, first_b = left
    second_a, second_b = right
    return (first_a * second_a, second_a * first_b + second_b)


def pair_folder(normed, pieces):
    return (
        jnp.dot(normed, pieces[0], preferred_element_type=jnp.float32),
        jnp.dot(normed, pieces[1], preferred_element_type=jnp.float32),
    )


def gathered_layer(
    tokens,
    mixer_norm_gain,
    recurrence_branch_weight,
    output_gate_projection,
    recurrence_conv_taps,
    recurrence_gate_map,
    input_gate_map,
    channel_decay_rate,
    position_log_decay,
    mixer_output_weight,
    feedforward_norm_gain,
    gate_up_weight,
    value_up_weight,
    gate_conv_taps,
    value_conv_taps,
    down_projection_weight,
):
    row_count = tokens.shape[0]
    local_width = recurrence_branch_weight.shape[1]
    local_heads = recurrence_gate_map.shape[0]
    head_size = recurrence_gate_map.shape[1]
    whole_rows = lax.all_gather(tokens, "tp", axis=1, tiled=True)
    normed = rms_normed(whole_rows, mixer_norm_gain)
    branch_sum, outgate_sum = pair_folder(
        normed,
        (
            lax.all_gather(recurrence_branch_weight, "fs", axis=0, tiled=True),
            lax.all_gather(output_gate_projection, "fs", axis=0, tiled=True),
        ),
    )
    branch = branch_sum.astype(jnp.bfloat16)
    outgate = outgate_sum.astype(jnp.bfloat16)
    conv = causal_conv(branch, recurrence_conv_taps).astype(jnp.bfloat16)
    grouped = conv.reshape(row_count, local_heads, head_size)
    recurrence_scan = jax.nn.sigmoid(
        jnp.einsum(
            "rhi,hij->rhj", grouped, recurrence_gate_map, preferred_element_type=jnp.float32
        ).reshape(row_count, local_width)
    )
    inner = jax.nn.sigmoid(
        jnp.einsum(
            "rhi,hij->rhj", grouped, input_gate_map, preferred_element_type=jnp.float32
        ).reshape(row_count, local_width)
    )
    log_alpha = (
        -DECAY_RATE_GAIN * recurrence_scan * channel_decay_rate[None, :] + position_log_decay
    )
    drive = jnp.sqrt(-jnp.expm1(2.0 * log_alpha)) * inner * conv.astype(jnp.float32)
    shape3 = (row_count // SEQ_LEN, SEQ_LEN, local_width)
    unused, state = lax.associative_scan(
        combine, (jnp.exp(log_alpha).reshape(shape3), drive.reshape(shape3)), axis=1
    )
    state = state.reshape(row_count, local_width)
    mixed = (state * jax.nn.gelu(outgate.astype(jnp.float32))).astype(jnp.bfloat16)
    mixer_terms = jnp.dot(
        mixed,
        lax.all_gather(mixer_output_weight, "fs", axis=1, tiled=True),
        preferred_element_type=jnp.float32,
    )
    mixer_terms = mixer_terms.astype(jnp.bfloat16).astype(jnp.float32)
    mixer_whole = lax.psum(mixer_terms.astype(jnp.bfloat16), "tp").astype(jnp.float32)
    whole_after = (whole_rows.astype(jnp.float32) + mixer_whole).astype(jnp.bfloat16)
    normed2 = rms_normed(whole_after, feedforward_norm_gain)
    gate_whole, value_whole = (
        lax.all_gather(gate_up_weight, "fs", axis=0, tiled=True),
        lax.all_gather(value_up_weight, "fs", axis=0, tiled=True),
    )
    gate_sum = jnp.dot(normed2, gate_whole, preferred_element_type=jnp.float32)
    value_sum = jnp.dot(normed2, value_whole, preferred_element_type=jnp.float32)
    gate_half = gate_sum.astype(jnp.bfloat16)
    value_half = value_sum.astype(jnp.bfloat16)
    hidden = (
        jax.nn.silu(causal_conv(gate_half, gate_conv_taps))
        * causal_conv(value_half, value_conv_taps)
    ).astype(jnp.bfloat16)
    channel_terms = jnp.dot(
        hidden,
        lax.all_gather(down_projection_weight, "fs", axis=1, tiled=True),
        preferred_element_type=jnp.float32,
    )
    channel_terms = channel_terms.astype(jnp.bfloat16).astype(jnp.float32)
    channel_share = lax.psum_scatter(
        channel_terms.astype(jnp.bfloat16), "tp", scatter_dimension=1, tiled=True
    ).astype(jnp.float32)
    share_width = channel_share.shape[1]
    residual_share = lax.dynamic_slice_in_dim(
        whole_after, lax.axis_index("tp") * share_width, share_width, 1
    )
    return (residual_share.astype(jnp.float32) + channel_share).astype(jnp.bfloat16)


VMEM = pl.BlockSpec(memory_space=pltpu.VMEM)
SMEM = pl.BlockSpec(memory_space=pltpu.SMEM)
ANY = pl.BlockSpec(memory_space=pl.ANY)
BUDGET = 56 * 1024 * 1024
NT = (((1,), (1,)), ((), ()))


def shifted(values, size, step):
    return lax.ppermute(values, "z", [(k, (k + step) % size) for k in range(size)])


def square_gather(values):
    half = values.shape[0] // 2
    across = [(k, k ^ 1) for k in range(4)]
    along = [(k, k ^ 2) for k in range(4)]
    first = lax.ppermute(values, "p", across)
    second = lax.ppermute(values, "p", along)
    top = lax.ppermute(second[:half], "p", across)
    bottom = lax.ppermute(first[half:], "p", along)
    return [values, first, second, top, bottom]


def piece_slots(depth, half):
    return [(4 * s + m, row) for s in range(depth) for m, row in ((0, 0), (1, 0), (2, 0), (3, 0), (3, half))]


def earlier(values, steps, row):
    return jnp.where(row >= steps, pltpu.roll(values, steps, 0), 0.0)


def convolved(values, taps, row):
    width = taps.shape[0]
    summed = values * taps[width - 1 : width]
    for steps in range(1, width):
        summed = summed + earlier(values, steps, row) * taps[width - 1 - steps : width - steps]
    return summed


def minus_expm1(value):
    series = 1.0 + value * (1.0 / 6.0)
    for order in (5.0, 4.0, 3.0, 2.0):
        series = 1.0 + value * (1.0 / order) * series
    return jnp.where(value > -0.25, -value * series, 1.0 - jnp.exp(value))


def mixer_kernel(slots, chunk, places, tok_own, tok_other, gain_own, gain_other, taps, maps, rate, decay, *rest):
    count = len(slots)
    pieces, (out_own, out_other), (wall, sums_ref, mixed_ref, sem) = (
        rest[:count],
        rest[count : count + 2],
        rest[count + 2 :],
    )
    half = tok_own.shape[1]
    local = rate.shape[1]
    copies = []
    for n, (slot, row) in enumerate(slots):
        at = pl.multiple_of(places[1 + slot] * chunk + row, 16)
        copy = pltpu.make_async_copy(
            pieces[n], wall.at[pl.ds(at, pieces[n].shape[0]), :], sem.at[n]
        )
        copy.start()
        copies.append(copy)
    own = tok_own[...].astype(jnp.float32)
    other = tok_other[...].astype(jnp.float32)
    mean = (
        jnp.sum(own * own, axis=1, keepdims=True) + jnp.sum(other * other, axis=1, keepdims=True)
    ) / (2 * half)
    factor = lax.rsqrt(mean + EPS)
    own = (own * factor * gain_own[...].astype(jnp.float32)).astype(jnp.bfloat16)
    other = (other * factor * gain_other[...].astype(jnp.float32)).astype(jnp.bfloat16)
    for copy in copies:
        copy.wait()
    at_own = pl.multiple_of(places[0] * half, 128)
    at_other = pl.multiple_of((1 - places[0]) * half, 128)
    sums_ref[...] = (
        jnp.dot(own, wall[pl.ds(at_own, half), : 2 * local], preferred_element_type=jnp.float32)
        + jnp.dot(other, wall[pl.ds(at_other, half), : 2 * local], preferred_element_type=jnp.float32)
    ).astype(jnp.bfloat16)
    rows = own.shape[0]
    block = maps.shape[1]
    row = lax.broadcasted_iota(jnp.int32, (rows, block), 0) % SEQ_LEN
    for group in range(local // block):
        lanes = slice(block * group, block * (group + 1))
        branch = sums_ref[:, lanes].astype(jnp.float32)
        conv = convolved(branch, taps[:, lanes].astype(jnp.float32), row).astype(jnp.bfloat16)
        gates = jnp.dot(conv, maps[group], preferred_element_type=jnp.float32)
        recur = jax.nn.sigmoid(gates[:, :block])
        inner = jax.nn.sigmoid(gates[:, block:])
        loga = -DECAY_RATE_GAIN * recur * rate[:, lanes] + decay[:, lanes]
        state = jnp.sqrt(minus_expm1(2.0 * loga)) * inner * conv.astype(jnp.float32)
        keep = jnp.exp(loga)
        steps = 1
        while steps < SEQ_LEN:
            state = keep * earlier(state, steps, row) + state
            if 2 * steps < SEQ_LEN:
                keep = keep * jnp.where(row >= steps, pltpu.roll(keep, steps, 0), 1.0)
            steps *= 2
        gate = sums_ref[:, local + block * group : local + block * (group + 1)].astype(jnp.float32)
        mixed_ref[:, lanes] = (state * jax.nn.gelu(gate)).astype(jnp.bfloat16)
    mixed = mixed_ref[...]
    for out, at in ((out_own, at_own), (out_other, at_other)):
        out[...] = lax.dot_general(
            mixed, wall[pl.ds(at, half), 2 * local :], NT, preferred_element_type=jnp.float32
        ).astype(jnp.bfloat16)


def up_kernel(slots, chunk, depth, full, places, *rest):
    count = len(slots)
    owns, others, taps = rest[:depth], rest[depth : 2 * depth], rest[2 * depth]
    pieces = rest[2 * depth + 1 : 2 * depth + 1 + count]
    hidden, wall, sem = rest[2 * depth + 1 + count :]
    copies = []
    for n, (slot, row) in enumerate(slots):
        at = pl.multiple_of(places[1 + slot] * chunk + row, 16)
        copy = pltpu.make_async_copy(
            pieces[n], wall.at[pl.ds(at, pieces[n].shape[0]), :], sem.at[n]
        )
        copy.start()
        copies.append(copy)
    for copy in copies:
        copy.wait()
    rows, half = owns[0].shape
    units = hidden.shape[1]
    at_own = pl.multiple_of(places[0] * half, 128)
    at_other = pl.multiple_of((1 - places[0]) * half, 128)
    row = lax.broadcasted_iota(jnp.int32, (rows, 2 * units), 0) % SEQ_LEN
    for s in range(depth):
        sums = jnp.dot(
            owns[s][...], wall[pl.ds(at_own, half), :], preferred_element_type=jnp.float32
        ) + jnp.dot(others[s][...], wall[pl.ds(at_other, half), :], preferred_element_type=jnp.float32)
        conv = convolved(
            sums.astype(jnp.bfloat16).astype(jnp.float32), taps[...].astype(jnp.float32), row
        )
        hidden[rows * s : rows * (s + 1), :full] = (
            jax.nn.silu(conv[:, :full]) * conv[:, full : 2 * full]
        ).astype(jnp.bfloat16)
        if full < units:
            hidden[rows * s : rows * (s + 1), full:] = (
                jax.nn.silu(conv[:, 2 * full : full + units]) * conv[:, full + units :]
            ).astype(jnp.bfloat16)


def down_kernel(slots, chunk, depth, places, hidden, *rest):
    count = len(slots)
    pieces = rest[:count]
    kept, given = rest[count : count + depth], rest[count + depth : count + 2 * depth]
    wall, sem = rest[count + 2 * depth :]
    copies = []
    for n, (slot, row) in enumerate(slots):
        at = pl.multiple_of(places[1 + slot] * chunk, 128)
        copy = pltpu.make_async_copy(
            pieces[n], wall.at[pl.ds(row, pieces[n].shape[0]), pl.ds(at, chunk)], sem.at[n]
        )
        copy.start()
        copies.append(copy)
    for copy in copies:
        copy.wait()
    rows, half = kept[0].shape
    at_own = pl.multiple_of(places[0] * half, 128)
    at_other = pl.multiple_of((1 - places[0]) * half, 128)
    for s in range(depth):
        left = hidden[rows * s : rows * (s + 1), :]
        for out, at in ((given[s], at_other), (kept[s], at_own)):
            out[...] = jnp.dot(
                left, wall[:, pl.ds(at, half)], preferred_element_type=jnp.float32
            ).astype(jnp.bfloat16)


def split_layer(
    depth,
    tokens,
    mixer_norm_gain,
    recurrence_branch_weight,
    output_gate_projection,
    recurrence_conv_taps,
    recurrence_gate_map,
    input_gate_map,
    channel_decay_rate,
    position_log_decay,
    mixer_output_weight,
    feedforward_norm_gain,
    gate_up_weight,
    value_up_weight,
    gate_conv_taps,
    value_conv_taps,
    down_projection_weight,
):
    rows, half = tokens.shape
    local = recurrence_branch_weight.shape[1]
    heads, head_size = recurrence_gate_map.shape[:2]
    chunk = recurrence_branch_weight.shape[0]
    units = gate_up_weight.shape[1] // depth
    full = units // 128 * 128
    z, p, c = lax.axis_index("z"), lax.axis_index("p"), lax.axis_index("c")
    swap = [(0, 1), (1, 0)]
    places = jnp.stack(
        [c] + [((z - s) % depth) * 4 + (p ^ m) for s in range(depth) for m in range(4)]
    ).astype(jnp.int32)

    def swapped(values):
        return lax.ppermute(values, "c", swap)

    def by_core(vector):
        pair = vector.reshape(2, 1, half)
        return (
            lax.dynamic_index_in_dim(pair, c, 0, False),
            lax.dynamic_index_in_dim(pair, 1 - c, 0, False),
        )

    tokens_other = swapped(tokens)

    mixer_piece = jnp.concatenate(
        [recurrence_branch_weight, output_gate_projection, mixer_output_weight.T], axis=1
    )
    mixer_pieces = []
    for s in range(depth):
        piece = mixer_piece if s == 0 else shifted(mixer_piece, depth, s)
        mixer_pieces += square_gather(piece)

    def packed(gate, value, k):
        lo, mid, hi = units * k, units * k + full, units * (k + 1)
        return jnp.concatenate([gate[:, lo:mid], value[:, lo:mid], gate[:, mid:hi], value[:, mid:hi]], axis=1)

    up_blocks = jnp.stack([packed(gate_up_weight, value_up_weight, k) for k in range(depth)])
    down_blocks = down_projection_weight.reshape(depth, units, chunk)
    up_parts, down_parts = [], []
    for s in range(depth):
        up = lax.dynamic_index_in_dim(up_blocks, (z + s) % depth, 0, False)
        up_parts.append(up if s == 0 else shifted(up, depth, s))
    for s in range(depth):
        down = lax.dynamic_index_in_dim(down_blocks, (z + s) % depth, 0, False)
        down_parts.append(down if s == 0 else shifted(down, depth, s))
    up_pieces, down_pieces = [], []
    for part in up_parts:
        up_pieces += square_gather(part)
    for part in down_parts:
        down_pieces += square_gather(part)

    group = 256 // head_size
    def diagonal(maps):
        eye = jnp.eye(group, dtype=maps.dtype)
        spread = maps.reshape(heads // group, group, head_size, 1, head_size) * eye[None, :, None, :, None]
        return spread.reshape(heads // group, 256, 256)

    maps = jnp.concatenate([diagonal(recurrence_gate_map), diagonal(input_gate_map)], axis=2)
    gain_own, gain_other = by_core(mixer_norm_gain)
    slots = piece_slots(depth, chunk // 2)
    mine = jax.ShapeDtypeStruct((rows, half), jnp.bfloat16)
    mine_own, mine_other = pl.pallas_call(
        functools.partial(mixer_kernel, slots, chunk),
        out_shape=(mine, mine),
        in_specs=[SMEM] + [VMEM] * 8 + [ANY] * len(slots),
        out_specs=(VMEM, VMEM),
        scratch_shapes=[
            pltpu.VMEM((2 * half, 3 * local), jnp.bfloat16),
            pltpu.VMEM((rows, 2 * local), jnp.bfloat16),
            pltpu.VMEM((rows, local), jnp.bfloat16),
            pltpu.SemaphoreType.DMA((len(slots),)),
        ],
        compiler_params=pltpu.CompilerParams(vmem_limit_bytes=BUDGET),
        name="mixer",
    )(
        places,
        tokens,
        tokens_other,
        gain_own,
        gain_other,
        recurrence_conv_taps,
        maps,
        channel_decay_rate[None, :],
        position_log_decay,
        *mixer_pieces,
    )
    theirs_own, theirs_other = swapped(mine_other), swapped(mine_own)

    def added(left, first, second):
        return (left.astype(jnp.float32) + (first.astype(jnp.float32) + second.astype(jnp.float32))).astype(
            jnp.bfloat16
        )

    after_own = added(tokens, mine_own, theirs_own)
    after_other = added(tokens_other, mine_other, theirs_other)
    wide_own, wide_other = after_own.astype(jnp.float32), after_other.astype(jnp.float32)
    mean = (
        jnp.sum(wide_own * wide_own, axis=1, keepdims=True)
        + jnp.sum(wide_other * wide_other, axis=1, keepdims=True)
    ) / (2 * half)
    factor = lax.rsqrt(mean + EPS)
    gain_own, gain_other = by_core(feedforward_norm_gain)
    normed_own = (wide_own * factor * gain_own.astype(jnp.float32)).astype(jnp.bfloat16)
    normed_other = (wide_other * factor * gain_other.astype(jnp.float32)).astype(jnp.bfloat16)
    owns = [normed_own] + [shifted(normed_own, depth, s) for s in range(1, depth)]
    others = [normed_other] + [swapped(owns[s]) for s in range(1, depth)]

    taps = packed(
        lax.dynamic_slice_in_dim(gate_conv_taps, z * units, units, 1),
        lax.dynamic_slice_in_dim(value_conv_taps, z * units, units, 1),
        0,
    )
    hidden = pl.pallas_call(
        functools.partial(up_kernel, slots, chunk, depth, full),
        out_shape=jax.ShapeDtypeStruct((depth * rows, units), jnp.bfloat16),
        in_specs=[SMEM] + [VMEM] * (2 * depth + 1) + [ANY] * len(slots),
        out_specs=VMEM,
        scratch_shapes=[
            pltpu.VMEM((2 * half, 2 * units), jnp.bfloat16),
            pltpu.SemaphoreType.DMA((len(slots),)),
        ],
        compiler_params=pltpu.CompilerParams(vmem_limit_bytes=BUDGET),
        name="up",
    )(places, *owns, *others, taps, *up_pieces)
    slots = piece_slots(depth, units // 2)
    products = pl.pallas_call(
        functools.partial(down_kernel, slots, chunk, depth),
        out_shape=(mine,) * (2 * depth),
        in_specs=[SMEM, VMEM] + [ANY] * len(slots),
        out_specs=(VMEM,) * (2 * depth),
        scratch_shapes=[
            pltpu.VMEM((units, 2 * half), jnp.bfloat16),
            pltpu.SemaphoreType.DMA((len(slots),)),
        ],
        compiler_params=pltpu.CompilerParams(vmem_limit_bytes=BUDGET),
        name="down",
    )(places, hidden, *down_pieces)
    total = None
    for s in range(depth):
        joined = products[s].astype(jnp.float32) + swapped(products[depth + s]).astype(jnp.float32)
        if s > 0:
            joined = shifted(joined.astype(jnp.bfloat16), depth, depth - s).astype(jnp.float32)
        total = joined if total is None else total + joined
    return (after_own.astype(jnp.float32) + total).astype(jnp.bfloat16)


def solution(mesh):
    placed = (
        P("fs", "tp"),
        P(),
        P("fs", "tp"),
        P("fs", "tp"),
        P(None, "tp"),
        P("tp", None, None),
        P("tp", None, None),
        P("tp"),
        P("fs", "tp"),
        P("tp", "fs"),
        P(),
        P("fs", "tp"),
        P("fs", "tp"),
        P(None, "tp"),
        P(None, "tp"),
        P("tp", "fs"),
    )
    shards, cores = mesh.shape["fs"], mesh.shape["tp"]
    if cores != 2 or shards % 4 != 0 or shards // 4 > 4:
        return jax.shard_map(
            gathered_layer, mesh=mesh, in_specs=placed, out_specs=P("fs", "tp"), check_vma=False
        )
    depth = shards // 4
    finer = Mesh(mesh.devices.reshape(depth, 4, cores), ("z", "p", "c"))
    names = {"fs": ("z", "p"), "tp": "c", None: None}
    split = tuple(P(*[names[name] for name in spec]) for spec in placed)
    step = jax.shard_map(
        functools.partial(split_layer, depth),
        mesh=finer,
        in_specs=split,
        out_specs=P(("z", "p"), "c"),
        check_vma=False,
    )
    return step
```

```python
import functools

import jax
import jax.numpy as jnp
from jax import lax
from jax.experimental import pallas as pl
from jax.experimental.pallas import tpu as pltpu
from jax.sharding import Mesh
from jax.sharding import PartitionSpec as P

SEQ_LEN = 64


EPS = 1e-06
DECAY_RATE_GAIN = 8.0


def rms_normed(values, gain):
    wide = values.astype(jnp.float32)
    factor = lax.rsqrt(jnp.mean(wide * wide, axis=-1, keepdims=True) + EPS)
    return (wide * factor * gain.astype(jnp.float32)).astype(jnp.bfloat16)


def causal_conv(values, kernel):
    width = kernel.shape[0]
    row_count, channels = values.shape
    grouped = values.astype(jnp.float32).reshape(row_count // SEQ_LEN, SEQ_LEN, channels)
    padded = jnp.pad(grouped, ((0, 0), (width - 1, 0), (0, 0)))
    summed = padded[:, 0:SEQ_LEN] * kernel[0].astype(jnp.float32)
    for offset in range(1, width):
        summed = summed + padded[:, offset : offset + SEQ_LEN] * kernel[offset].astype(jnp.float32)
    return summed.reshape(row_count, channels)


def combine(left, right):
    first_a, first_b = left
    second_a, second_b = right
    return (first_a * second_a, second_a * first_b + second_b)


def pair_folder(normed, pieces):
    return (
        jnp.dot(normed, pieces[0], preferred_element_type=jnp.float32),
        jnp.dot(normed, pieces[1], preferred_element_type=jnp.float32),
    )


def gathered_layer(
    tokens,
    mixer_norm_gain,
    recurrence_branch_weight,
    output_gate_projection,
    recurrence_conv_taps,
    recurrence_gate_map,
    input_gate_map,
    channel_decay_rate,
    position_log_decay,
    mixer_output_weight,
    feedforward_norm_gain,
    gate_up_weight,
    value_up_weight,
    gate_conv_taps,
    value_conv_taps,
    down_projection_weight,
):
    row_count = tokens.shape[0]
    local_width = recurrence_branch_weight.shape[1]
    local_heads = recurrence_gate_map.shape[0]
    head_size = recurrence_gate_map.shape[1]
    whole_rows = lax.all_gather(tokens, "tp", axis=1, tiled=True)
    normed = rms_normed(whole_rows, mixer_norm_gain)
    branch_sum, outgate_sum = pair_folder(
        normed,
        (
            lax.all_gather(recurrence_branch_weight, "fs", axis=0, tiled=True),
            lax.all_gather(output_gate_projection, "fs", axis=0, tiled=True),
        ),
    )
    branch = branch_sum.astype(jnp.bfloat16)
    outgate = outgate_sum.astype(jnp.bfloat16)
    conv = causal_conv(branch, recurrence_conv_taps).astype(jnp.bfloat16)
    grouped = conv.reshape(row_count, local_heads, head_size)
    recurrence_scan = jax.nn.sigmoid(
        jnp.einsum(
            "rhi,hij->rhj", grouped, recurrence_gate_map, preferred_element_type=jnp.float32
        ).reshape(row_count, local_width)
    )
    inner = jax.nn.sigmoid(
        jnp.einsum(
            "rhi,hij->rhj", grouped, input_gate_map, preferred_element_type=jnp.float32
        ).reshape(row_count, local_width)
    )
    log_alpha = (
        -DECAY_RATE_GAIN * recurrence_scan * channel_decay_rate[None, :] + position_log_decay
    )
    drive = jnp.sqrt(-jnp.expm1(2.0 * log_alpha)) * inner * conv.astype(jnp.float32)
    shape3 = (row_count // SEQ_LEN, SEQ_LEN, local_width)
    _, state = lax.associative_scan(
        combine, (jnp.exp(log_alpha).reshape(shape3), drive.reshape(shape3)), axis=1
    )
    state = state.reshape(row_count, local_width)
    mixed = (state * jax.nn.gelu(outgate.astype(jnp.float32))).astype(jnp.bfloat16)
    mixer_terms = jnp.dot(
        mixed,
        lax.all_gather(mixer_output_weight, "fs", axis=1, tiled=True),
        preferred_element_type=jnp.float32,
    )
    mixer_terms = mixer_terms.astype(jnp.bfloat16).astype(jnp.float32)
    mixer_whole = lax.psum(mixer_terms.astype(jnp.bfloat16), "tp").astype(jnp.float32)
    whole_after = (whole_rows.astype(jnp.float32) + mixer_whole).astype(jnp.bfloat16)
    normed2 = rms_normed(whole_after, feedforward_norm_gain)
    gate_whole, value_whole = (
        lax.all_gather(gate_up_weight, "fs", axis=0, tiled=True),
        lax.all_gather(value_up_weight, "fs", axis=0, tiled=True),
    )
    gate_sum = jnp.dot(normed2, gate_whole, preferred_element_type=jnp.float32)
    value_sum = jnp.dot(normed2, value_whole, preferred_element_type=jnp.float32)
    gate_half = gate_sum.astype(jnp.bfloat16)
    value_half = value_sum.astype(jnp.bfloat16)
    hidden = (
        jax.nn.silu(causal_conv(gate_half, gate_conv_taps))
        * causal_conv(value_half, value_conv_taps)
    ).astype(jnp.bfloat16)
    channel_terms = jnp.dot(
        hidden,
        lax.all_gather(down_projection_weight, "fs", axis=1, tiled=True),
        preferred_element_type=jnp.float32,
    )
    channel_terms = channel_terms.astype(jnp.bfloat16).astype(jnp.float32)
    channel_share = lax.psum_scatter(
        channel_terms.astype(jnp.bfloat16), "tp", scatter_dimension=1, tiled=True
    ).astype(jnp.float32)
    share_width = channel_share.shape[1]
    residual_share = lax.dynamic_slice_in_dim(
        whole_after, lax.axis_index("tp") * share_width, share_width, 1
    )
    return (residual_share.astype(jnp.float32) + channel_share).astype(jnp.bfloat16)


VMEM = pl.BlockSpec(memory_space=pltpu.VMEM)
SMEM = pl.BlockSpec(memory_space=pltpu.SMEM)
ANY = pl.BlockSpec(memory_space=pl.ANY)
BUDGET = 56 * 1024 * 1024
SMALL = 24 * 1024 * 1024
NT = (((1,), (1,)), ((), ()))


def traded(values, axis, size, m):
    return lax.ppermute(values, axis, [(k, k ^ m) for k in range(size)])


def line_gather(values, depth):
    if depth == 2:
        return [values, traded(values, "z", depth, 1)]
    near = traded(values, "z", depth, 1)
    far = traded(values, "z", depth, 2)
    inner = lax.ppermute(values, "z", [(1, 2), (2, 1)])
    outer = lax.ppermute(far, "z", [(1, 0), (2, 3)])
    return [values, near, far, inner + outer]


def line_scatter(blocks, depth):
    near = traded(blocks[1], "z", depth, 1).astype(jnp.float32)
    total = blocks[0].astype(jnp.float32) + near
    if depth == 2:
        return total
    outer = lax.ppermute(blocks[3], "z", [(0, 1), (3, 2)])
    inner = lax.ppermute(blocks[3], "z", [(1, 2), (2, 1)])
    through = (blocks[2].astype(jnp.float32) + outer.astype(jnp.float32)).astype(jnp.bfloat16)
    far = traded(through, "z", depth, 2)
    return total + inner.astype(jnp.float32) + far.astype(jnp.float32)


def square_gather(parts):
    found = []
    for s, part in enumerate(parts):
        across = traded(part, "p", 4, 1)
        along = traded(part, "p", 4, 2)
        if s % 2 == 0:
            far = traded(along, "p", 4, 1)
        else:
            far = traded(across, "p", 4, 2)
        found += [part, across, along, far]
    return found


def earlier(values, steps, row):
    return jnp.where(row >= steps, pltpu.roll(values, steps, 0), 0.0)


def convolved(values, taps, row):
    width = taps.shape[0]
    summed = values * taps[width - 1 : width]
    for steps in range(1, width):
        summed = summed + earlier(values, steps, row) * taps[width - 1 - steps : width - steps]
    return summed


def minus_expm1(value):
    series = 1.0 + value * (1.0 / 6.0)
    for order in (5.0, 4.0, 3.0, 2.0):
        series = 1.0 + value * (1.0 / order) * series
    return jnp.where(value > -0.25, -value * series, 1.0 - jnp.exp(value))


def normed_halves(own, other, gains, core):
    own, other = own.astype(jnp.float32), other.astype(jnp.float32)
    mean = (
        jnp.sum(own * own, axis=1, keepdims=True) + jnp.sum(other * other, axis=1, keepdims=True)
    ) / (2 * own.shape[1])
    factor = lax.rsqrt(mean + EPS)
    return (
        (own * factor * gains[core].astype(jnp.float32)).astype(jnp.bfloat16),
        (other * factor * gains[1 - core].astype(jnp.float32)).astype(jnp.bfloat16),
    )


def join_kernel(places, tok_own, tok_other, mine_own, mine_other, theirs_own, theirs_other, gains, after_own, own, other):
    def added(left, first, second):
        return (
            left[...].astype(jnp.float32)
            + (first[...].astype(jnp.float32) + second[...].astype(jnp.float32))
        ).astype(jnp.bfloat16)

    mine = added(tok_own, mine_own, theirs_own)
    after_own[...] = mine
    own[...], other[...] = normed_halves(
        mine, added(tok_other, mine_other, theirs_other), gains, places[0]
    )


def pack_kernel(depth, places, gate, value, down, *rest):
    ups, downs, (packed, sem) = rest[:depth], rest[depth : 2 * depth], rest[2 * depth :]
    units = gate.shape[1] // depth
    copies = []
    for s in range(depth):
        at = pl.multiple_of((places[1] ^ s) * units, 16)
        copies.append(pltpu.make_async_copy(down.at[pl.ds(at, units), :], downs[s], sem.at[depth + s]))
        copies[-1].start()
    for k in range(depth):
        for low, size in tiles(units):
            lanes = slice(units * k + low, units * k + low + size)
            packed[k, :, 2 * low : 2 * low + size] = gate[:, lanes]
            packed[k, :, 2 * low + size : 2 * low + 2 * size] = value[:, lanes]
    for s in range(depth):
        copies.append(pltpu.make_async_copy(packed.at[places[1] ^ s], ups[s], sem.at[s]))
        copies[-1].start()
    for copy in copies:
        copy.wait()


def tiles(units):
    return [(low, min(128, units - low)) for low in range(0, units, 128)]


def hidden_tiles(left, wall, taps, out):
    rows = left.shape[0]
    row = lax.broadcasted_iota(jnp.int32, (rows, 256), 0) % SEQ_LEN
    for low, size in tiles(out.shape[1]):
        lanes = slice(2 * low, 2 * low + 2 * size)
        sums = jnp.dot(left[...], wall[:, lanes], preferred_element_type=jnp.float32)
        conv = convolved(
            sums.astype(jnp.bfloat16).astype(jnp.float32),
            taps[:, lanes].astype(jnp.float32),
            row[:, : 2 * size],
        )
        out[:, low : low + size] = (jax.nn.silu(conv[:, :size]) * conv[:, size:]).astype(jnp.bfloat16)


def started(copies):
    for copy in copies:
        copy.start()
    return copies


def gather_rows(pieces, wall, places, chunk):
    for n, piece in enumerate(pieces):
        wall[pl.ds(pl.multiple_of(places[2 + n] * chunk, chunk), chunk), :] = piece[...]


def near_kernel(count, chunk, depth, places, taps, *rest):
    owns, others, pieces = rest[:depth], rest[depth : 2 * depth], rest[2 * depth : 2 * depth + count]
    hidden, left, wall = rest[2 * depth + count :]
    rows, half = owns[0].shape
    gather_rows(pieces, wall, places, chunk)
    for k in range(depth):
        for block, side in ((owns[k], places[0]), (others[k], 1 - places[0])):
            left[rows * k : rows * (k + 1), pl.ds(pl.multiple_of(side * half, 128), half)] = block[...]
    hidden_tiles(left, wall, taps.at[places[1]], hidden)


def down_kernel(count, chunk, blocks, given_to, places, *rest):
    hiddens, pieces = rest[:given_to], rest[given_to : given_to + count]
    outs, (wall, now, sem) = rest[given_to + count : -3], rest[-3:]
    rows, half = outs[0].shape
    for n, piece in enumerate(pieces):
        wall[n] = piece[...]
    core, z, p = places[0], places[1], places[2] % 4
    copies = []
    for k, (which, block) in enumerate(blocks):
        left = hiddens[which][rows * block : rows * (block + 1), :]
        for j, side in enumerate((1 - core, core)):
            n = 2 * k + j
            for low in range(0, half, 256):
                block_at = side * (half // chunk) + low // chunk
                right = jnp.concatenate(
                    [
                        wall[4 * (((block_at + i) // 4) ^ z) + (((block_at + i) % 4) ^ p)]
                        for i in range(256 // chunk)
                    ],
                    axis=1,
                )
                now[n, :, low : low + 256] = jnp.dot(
                    left, right, preferred_element_type=jnp.float32
                ).astype(jnp.bfloat16)
            copies += started([pltpu.make_async_copy(now.at[n], outs[n], sem.at[n])])
    for copy in copies:
        copy.wait()


def mixer_kernel(count, chunk, places, tok_own, tok_other, gains, taps, recur_map, input_map, rate, decay, *rest):
    pieces, (out_own, out_other), (wall, sums_ref, mixed_ref, maps) = (
        rest[:count],
        rest[count : count + 2],
        rest[count + 2 :],
    )
    half = tok_own.shape[1]
    local = rate.shape[1]
    gather_rows(pieces, wall, places, chunk)
    maps[...] = jnp.zeros_like(maps)
    block = maps.shape[1]
    size = recur_map.shape[1]
    for head in range(recur_map.shape[0]):
        group, low = divmod(head * size, block)
        maps[group, low : low + size, low : low + size] = recur_map[head]
        maps[group, low : low + size, block + low : block + low + size] = input_map[head]
    own, other = normed_halves(tok_own[...], tok_other[...], gains, places[0])
    at_own = pl.multiple_of(places[0] * half, 128)
    at_other = pl.multiple_of((1 - places[0]) * half, 128)
    sums_ref[...] = (
        jnp.dot(own, wall[pl.ds(at_own, half), : 2 * local], preferred_element_type=jnp.float32)
        + jnp.dot(other, wall[pl.ds(at_other, half), : 2 * local], preferred_element_type=jnp.float32)
    ).astype(jnp.bfloat16)
    rows = own.shape[0]
    row = lax.broadcasted_iota(jnp.int32, (rows, block), 0) % SEQ_LEN
    for group in range(local // block):
        lanes = slice(block * group, block * (group + 1))
        branch = sums_ref[:, lanes].astype(jnp.float32)
        conv = convolved(branch, taps[:, lanes].astype(jnp.float32), row).astype(jnp.bfloat16)
        gates = jnp.dot(conv, maps[group], preferred_element_type=jnp.float32)
        recur = jax.nn.sigmoid(gates[:, :block])
        inner = jax.nn.sigmoid(gates[:, block:])
        loga = -DECAY_RATE_GAIN * recur * rate[:, lanes] + decay[:, lanes]
        state = jnp.sqrt(minus_expm1(2.0 * loga)) * inner * conv.astype(jnp.float32)
        keep = jnp.exp(loga)
        steps = 1
        while steps < SEQ_LEN:
            state = keep * earlier(state, steps, row) + state
            if 2 * steps < SEQ_LEN:
                keep = keep * jnp.where(row >= steps, pltpu.roll(keep, steps, 0), 1.0)
            steps *= 2
        gate = sums_ref[:, local + block * group : local + block * (group + 1)].astype(jnp.float32)
        mixed_ref[:, lanes] = (state * jax.nn.gelu(gate)).astype(jnp.bfloat16)
    mixed = mixed_ref[...]
    for out, at in ((out_own, at_own), (out_other, at_other)):
        out[...] = lax.dot_general(
            mixed, wall[pl.ds(at, half), 2 * local :], NT, preferred_element_type=jnp.float32
        ).astype(jnp.bfloat16)


def split_layer(depth, *arrays):
    return split_layer_body(depth, *arrays)


def split_layer_body(
    depth,
    tokens,
    mixer_norm_gain,
    recurrence_branch_weight,
    output_gate_projection,
    recurrence_conv_taps,
    recurrence_gate_map,
    input_gate_map,
    channel_decay_rate,
    position_log_decay,
    mixer_output_weight,
    feedforward_norm_gain,
    gate_up_weight,
    value_up_weight,
    gate_conv_taps,
    value_conv_taps,
    down_projection_weight,
):
    rows, half = tokens.shape
    local = recurrence_branch_weight.shape[1]
    chunk = recurrence_branch_weight.shape[0]
    units = gate_up_weight.shape[1] // depth
    z, p, c = lax.axis_index("z"), lax.axis_index("p"), lax.axis_index("c")
    swap = [(0, 1), (1, 0)]
    places = jnp.stack(
        [c, z] + [(z ^ s) * 4 + (p ^ m) for s in range(depth) for m in range(4)]
    ).astype(jnp.int32)
    both_taps = jnp.stack(
        [
            jnp.concatenate(
                [
                    taps[:, units * k + low : units * k + low + size]
                    for low, size in tiles(units)
                    for taps in (gate_conv_taps, value_conv_taps)
                ],
                axis=1,
            )
            for k in range(depth)
        ]
    )

    def swapped(values):
        return lax.ppermute(values, "c", swap)

    tokens_other = swapped(tokens)

    mixer_piece = jnp.concatenate(
        [recurrence_branch_weight, output_gate_projection, mixer_output_weight.T], axis=1
    )
    mixer_parts = line_gather(mixer_piece, depth)
    mixer_parts[-1], places_used, both_taps = lax.optimization_barrier((mixer_parts[-1], places, both_taps))
    mixer_pieces = square_gather(mixer_parts)

    shares = pl.pallas_call(
        functools.partial(pack_kernel, depth),
        out_shape=(jax.ShapeDtypeStruct((chunk, 2 * units), jnp.bfloat16),) * depth
        + (jax.ShapeDtypeStruct((units, chunk), jnp.bfloat16),) * depth,
        in_specs=[SMEM, VMEM, VMEM, VMEM],
        out_specs=(ANY,) * (2 * depth),
        scratch_shapes=[
            pltpu.VMEM((depth, chunk, 2 * units), jnp.bfloat16),
            pltpu.SemaphoreType.DMA((2 * depth,)),
        ],
        compiler_params=pltpu.CompilerParams(vmem_limit_bytes=BUDGET),
        name="pack",
    )(places, gate_up_weight, value_up_weight, down_projection_weight)
    up_parts = [shares[s] if s == 0 else traded(shares[s], "z", depth, s) for s in range(depth)]
    down_parts = [shares[depth + s] if s == 0 else traded(shares[depth + s], "z", depth, s) for s in range(depth)]
    up_pieces = square_gather(up_parts)
    down_pieces = square_gather(down_parts)

    mine = jax.ShapeDtypeStruct((rows, half), jnp.bfloat16)
    mine_own, mine_other = pl.pallas_call(
        functools.partial(mixer_kernel, len(mixer_pieces), chunk),
        out_shape=(mine, mine),
        in_specs=[SMEM] + [VMEM] * (8 + len(mixer_pieces)),
        out_specs=(VMEM, VMEM),
        scratch_shapes=[
            pltpu.VMEM((2 * half, 3 * local), jnp.bfloat16),
            pltpu.VMEM((rows, 2 * local), jnp.bfloat16),
            pltpu.VMEM((rows, local), jnp.bfloat16),
            pltpu.VMEM((local // 256, 256, 512), jnp.bfloat16),
        ],
        compiler_params=pltpu.CompilerParams(vmem_limit_bytes=SMALL),
        name="mixer",
    )(
        places_used,
        tokens,
        tokens_other,
        mixer_norm_gain.reshape(2, 1, half),
        recurrence_conv_taps,
        recurrence_gate_map,
        input_gate_map,
        channel_decay_rate[None, :],
        position_log_decay,
        *mixer_pieces,
    )
    theirs_own, theirs_other = swapped(mine_other), swapped(mine_own)

    after_own, normed_own, normed_other = pl.pallas_call(
        join_kernel,
        out_shape=(mine,) * 3,
        in_specs=[SMEM] + [VMEM] * 7,
        out_specs=(VMEM,) * 3,
        name="join",
    )(
        places_used,
        tokens,
        tokens_other,
        mine_own,
        mine_other,
        theirs_own,
        theirs_other,
        feedforward_norm_gain.reshape(2, 1, half),
    )
    owns = line_gather(normed_own, depth)
    others = [normed_other] + [swapped(owns[s]) for s in range(1, depth)]

    count = len(up_pieces)

    def up(members):
        size = len(members)
        return pl.pallas_call(
            functools.partial(near_kernel, count, chunk, size),
            out_shape=jax.ShapeDtypeStruct((size * rows, units), jnp.bfloat16),
            in_specs=[SMEM] + [VMEM] * (1 + 2 * size + count),
            out_specs=VMEM,
            scratch_shapes=[
                pltpu.VMEM((size * rows, 2 * half), jnp.bfloat16),
                pltpu.VMEM((2 * half, 2 * units), jnp.bfloat16),
            ],
            compiler_params=pltpu.CompilerParams(vmem_limit_bytes=SMALL),
        )(places_used, both_taps, *[owns[s] for s in members], *[others[s] for s in members], *up_pieces)

    def down(early, late, members):
        hiddens = [early] if late is None else [early, late]
        blocks = [(1, 0) if s == depth - 1 else (0, s) for s in members]
        outs = pl.pallas_call(
            functools.partial(down_kernel, count, chunk, blocks, len(hiddens)),
            out_shape=(mine,) * (2 * len(members)),
            in_specs=[SMEM] + [VMEM] * (len(hiddens) + count),
            out_specs=(ANY,) * (2 * len(members)),
            scratch_shapes=[
                pltpu.VMEM((count, units, chunk), jnp.bfloat16),
                pltpu.VMEM((2 * len(members), rows, half), jnp.bfloat16),
                pltpu.SemaphoreType.DMA((2 * len(members),)),
            ],
            compiler_params=pltpu.CompilerParams(vmem_limit_bytes=SMALL),
        )(places_used, *hiddens, *down_pieces)
        return {s: (outs[2 * k + 1], outs[2 * k]) for k, s in enumerate(members)}

    hidden = up(list(range(depth - 1)))
    hidden_late = up([depth - 1])
    products = down(hidden, hidden_late, [*range(depth - 1, -1, -1)])
    blocks = []
    for s in range(depth):
        kept, given = products[s]
        block = kept.astype(jnp.float32) + swapped(given).astype(jnp.float32)
        blocks.append(block if s == 0 else block.astype(jnp.bfloat16))
    total = line_scatter(blocks, depth)
    return (after_own.astype(jnp.float32) + total).astype(jnp.bfloat16)


def solution(mesh):
    placed = (
        P("fs", "tp"),
        P(),
        P("fs", "tp"),
        P("fs", "tp"),
        P(None, "tp"),
        P("tp", None, None),
        P("tp", None, None),
        P("tp"),
        P("fs", "tp"),
        P("tp", "fs"),
        P(),
        P("fs", "tp"),
        P("fs", "tp"),
        P(None, "tp"),
        P(None, "tp"),
        P("tp", "fs"),
    )
    shards, cores = mesh.shape["fs"], mesh.shape["tp"]
    if cores != 2 or shards not in (8, 16):
        return jax.shard_map(
            gathered_layer, mesh=mesh, in_specs=placed, out_specs=P("fs", "tp"), check_vma=False
        )
    depth = shards // 4
    finer = Mesh(mesh.devices.reshape(depth, 4, cores), ("z", "p", "c"))
    names = {"fs": ("z", "p"), "tp": "c", None: None}
    split = tuple(P(*[names[name] for name in spec]) for spec in placed)
    return jax.shard_map(
        functools.partial(split_layer, depth),
        mesh=finer,
        in_specs=split,
        out_specs=P(("z", "p"), "c"),
        check_vma=False,
    )
```

```python
import functools

import jax
import jax.numpy as jnp
from jax import lax
from jax.experimental import pallas as pl
from jax.experimental.pallas import tpu as pltpu
from jax.sharding import Mesh
from jax.sharding import PartitionSpec as P

SEQ_LEN = 64


EPS = 1e-06
DECAY_RATE_GAIN = 8.0


def rms_normed(values, gain):
    wide = values.astype(jnp.float32)
    factor = lax.rsqrt(jnp.mean(wide * wide, axis=-1, keepdims=True) + EPS)
    return (wide * factor * gain.astype(jnp.float32)).astype(jnp.bfloat16)


def causal_conv(values, kernel):
    width = kernel.shape[0]
    row_count, channels = values.shape
    grouped = values.astype(jnp.float32).reshape(row_count // SEQ_LEN, SEQ_LEN, channels)
    padded = jnp.pad(grouped, ((0, 0), (width - 1, 0), (0, 0)))
    summed = padded[:, 0:SEQ_LEN] * kernel[0].astype(jnp.float32)
    for offset in range(1, width):
        summed = summed + padded[:, offset : offset + SEQ_LEN] * kernel[offset].astype(jnp.float32)
    return summed.reshape(row_count, channels)


def combine(left, right):
    first_a, first_b = left
    second_a, second_b = right
    return (first_a * second_a, second_a * first_b + second_b)


def pair_folder(normed, pieces):
    return (
        jnp.dot(normed, pieces[0], preferred_element_type=jnp.float32),
        jnp.dot(normed, pieces[1], preferred_element_type=jnp.float32),
    )


def gathered_layer(
    tokens,
    mixer_norm_gain,
    recurrence_branch_weight,
    output_gate_projection,
    recurrence_conv_taps,
    recurrence_gate_map,
    input_gate_map,
    channel_decay_rate,
    position_log_decay,
    mixer_output_weight,
    feedforward_norm_gain,
    gate_up_weight,
    value_up_weight,
    gate_conv_taps,
    value_conv_taps,
    down_projection_weight,
):
    row_count = tokens.shape[0]
    local_width = recurrence_branch_weight.shape[1]
    local_heads = recurrence_gate_map.shape[0]
    head_size = recurrence_gate_map.shape[1]
    whole_rows = lax.all_gather(tokens, "tp", axis=1, tiled=True)
    normed = rms_normed(whole_rows, mixer_norm_gain)
    branch_sum, outgate_sum = pair_folder(
        normed,
        (
            lax.all_gather(recurrence_branch_weight, "fs", axis=0, tiled=True),
            lax.all_gather(output_gate_projection, "fs", axis=0, tiled=True),
        ),
    )
    branch = branch_sum.astype(jnp.bfloat16)
    outgate = outgate_sum.astype(jnp.bfloat16)
    conv = causal_conv(branch, recurrence_conv_taps).astype(jnp.bfloat16)
    grouped = conv.reshape(row_count, local_heads, head_size)
    recurrence_scan = jax.nn.sigmoid(
        jnp.einsum(
            "rhi,hij->rhj", grouped, recurrence_gate_map, preferred_element_type=jnp.float32
        ).reshape(row_count, local_width)
    )
    inner = jax.nn.sigmoid(
        jnp.einsum(
            "rhi,hij->rhj", grouped, input_gate_map, preferred_element_type=jnp.float32
        ).reshape(row_count, local_width)
    )
    log_alpha = (
        -DECAY_RATE_GAIN * recurrence_scan * channel_decay_rate[None, :] + position_log_decay
    )
    drive = jnp.sqrt(-jnp.expm1(2.0 * log_alpha)) * inner * conv.astype(jnp.float32)
    shape3 = (row_count // SEQ_LEN, SEQ_LEN, local_width)
    _, state = lax.associative_scan(
        combine, (jnp.exp(log_alpha).reshape(shape3), drive.reshape(shape3)), axis=1
    )
    state = state.reshape(row_count, local_width)
    mixed = (state * jax.nn.gelu(outgate.astype(jnp.float32))).astype(jnp.bfloat16)
    mixer_terms = jnp.dot(
        mixed,
        lax.all_gather(mixer_output_weight, "fs", axis=1, tiled=True),
        preferred_element_type=jnp.float32,
    )
    mixer_terms = mixer_terms.astype(jnp.bfloat16).astype(jnp.float32)
    mixer_whole = lax.psum(mixer_terms.astype(jnp.bfloat16), "tp").astype(jnp.float32)
    whole_after = (whole_rows.astype(jnp.float32) + mixer_whole).astype(jnp.bfloat16)
    normed2 = rms_normed(whole_after, feedforward_norm_gain)
    gate_whole, value_whole = (
        lax.all_gather(gate_up_weight, "fs", axis=0, tiled=True),
        lax.all_gather(value_up_weight, "fs", axis=0, tiled=True),
    )
    gate_sum = jnp.dot(normed2, gate_whole, preferred_element_type=jnp.float32)
    value_sum = jnp.dot(normed2, value_whole, preferred_element_type=jnp.float32)
    gate_half = gate_sum.astype(jnp.bfloat16)
    value_half = value_sum.astype(jnp.bfloat16)
    hidden = (
        jax.nn.silu(causal_conv(gate_half, gate_conv_taps))
        * causal_conv(value_half, value_conv_taps)
    ).astype(jnp.bfloat16)
    channel_terms = jnp.dot(
        hidden,
        lax.all_gather(down_projection_weight, "fs", axis=1, tiled=True),
        preferred_element_type=jnp.float32,
    )
    channel_terms = channel_terms.astype(jnp.bfloat16).astype(jnp.float32)
    channel_share = lax.psum_scatter(
        channel_terms.astype(jnp.bfloat16), "tp", scatter_dimension=1, tiled=True
    ).astype(jnp.float32)
    share_width = channel_share.shape[1]
    residual_share = lax.dynamic_slice_in_dim(
        whole_after, lax.axis_index("tp") * share_width, share_width, 1
    )
    return (residual_share.astype(jnp.float32) + channel_share).astype(jnp.bfloat16)


VMEM = pl.BlockSpec(memory_space=pltpu.VMEM)
SMEM = pl.BlockSpec(memory_space=pltpu.SMEM)
ANY = pl.BlockSpec(memory_space=pl.ANY)
SMALL = 24 * 1024 * 1024
NT = (((1,), (1,)), ((), ()))


def traded(values, axis, size, m):
    return lax.ppermute(values, axis, [(k, k ^ m) for k in range(size)])


def line_gather(values, depth):
    if depth == 2:
        return [values, traded(values, "z", depth, 1)]
    near = traded(values, "z", depth, 1)
    far = traded(values, "z", depth, 2)
    inner = lax.ppermute(values, "z", [(1, 2), (2, 1)])
    outer = lax.ppermute(far, "z", [(1, 0), (2, 3)])
    return [values, near, far, inner + outer]


def line_scatter(blocks, depth):
    near = traded(blocks[1], "z", depth, 1).astype(jnp.float32)
    total = blocks[0].astype(jnp.float32) + near
    if depth == 2:
        return total
    outer = lax.ppermute(blocks[3], "z", [(0, 1), (3, 2)])
    inner = lax.ppermute(blocks[3], "z", [(1, 2), (2, 1)])
    middle = lax.optimization_barrier(blocks[2])
    direct = lax.ppermute(middle, "z", [(0, 2), (3, 1)])
    through = (middle.astype(jnp.float32) + outer.astype(jnp.float32)).astype(jnp.bfloat16)
    joined = lax.ppermute(through, "z", [(1, 3), (2, 0)])
    return total + inner.astype(jnp.float32) + (direct.astype(jnp.float32) + joined.astype(jnp.float32))


def square_gather(parts):
    found = []
    for s, part in enumerate(parts):
        across = traded(part, "p", 4, 1)
        along = traded(part, "p", 4, 2)
        if s % 2 == 0:
            far = traded(along, "p", 4, 1)
        else:
            far = traded(across, "p", 4, 2)
        found += [part, across, along, far]
    return found


def earlier(values, steps, row):
    return jnp.where(row >= steps, pltpu.roll(values, steps, 0), 0.0)


def convolved(values, taps, row):
    width = taps.shape[0]
    summed = values * taps[width - 1 : width]
    for steps in range(1, width):
        summed = summed + earlier(values, steps, row) * taps[width - 1 - steps : width - steps]
    return summed


def minus_expm1(value):
    series = 1.0 + value * (1.0 / 6.0)
    for order in (5.0, 4.0, 3.0, 2.0):
        series = 1.0 + value * (1.0 / order) * series
    return jnp.where(value > -0.25, -value * series, 1.0 - jnp.exp(value))


def normed_halves(own, other, gains, core):
    own, other = own.astype(jnp.float32), other.astype(jnp.float32)
    mean = (
        jnp.sum(own * own, axis=1, keepdims=True) + jnp.sum(other * other, axis=1, keepdims=True)
    ) / (2 * own.shape[1])
    factor = lax.rsqrt(mean + EPS)
    return (
        (own * factor * gains[core].astype(jnp.float32)).astype(jnp.bfloat16),
        (other * factor * gains[1 - core].astype(jnp.float32)).astype(jnp.bfloat16),
    )


def join_kernel(places, tok_own, tok_other, mine_own, mine_other, theirs_own, theirs_other, gains, after_own, own, other):
    def added(left, first, second):
        return (
            left[...].astype(jnp.float32)
            + (first[...].astype(jnp.float32) + second[...].astype(jnp.float32))
        ).astype(jnp.bfloat16)

    mine = added(tok_own, mine_own, theirs_own)
    after_own[...] = mine
    own[...], other[...] = normed_halves(
        mine, added(tok_other, mine_other, theirs_other), gains, places[0]
    )


def pack_kernel(depth, places, gate, value, down, *rest):
    ups, downs, (packed, sem) = rest[:depth], rest[depth : 2 * depth], rest[2 * depth :]
    units = gate.shape[1] // depth
    copies = []
    for s in range(depth):
        at = pl.multiple_of((places[1] ^ s) * units, 16)
        copies.append(pltpu.make_async_copy(down.at[pl.ds(at, units), :], downs[s], sem.at[depth + s]))
        copies[-1].start()
    for k in range(depth):
        for low, size in tiles(units):
            lanes = slice(units * k + low, units * k + low + size)
            packed[k, :, 2 * low : 2 * low + size] = gate[:, lanes]
            packed[k, :, 2 * low + size : 2 * low + 2 * size] = value[:, lanes]
    for s in range(depth):
        copies.append(pltpu.make_async_copy(packed.at[places[1] ^ s], ups[s], sem.at[s]))
        copies[-1].start()
    for copy in copies:
        copy.wait()


def tiles(units):
    return [(low, min(128, units - low)) for low in range(0, units, 128)]


def hidden_tiles(left, wall, taps, out):
    rows = left.shape[0]
    row = lax.broadcasted_iota(jnp.int32, (rows, 256), 0) % SEQ_LEN
    for low, size in tiles(out.shape[1]):
        lanes = slice(2 * low, 2 * low + 2 * size)
        sums = jnp.dot(left[...], wall[:, lanes], preferred_element_type=jnp.float32)
        conv = convolved(
            sums.astype(jnp.bfloat16).astype(jnp.float32),
            taps[:, lanes].astype(jnp.float32),
            row[:, : 2 * size],
        )
        out[:, low : low + size] = (jax.nn.silu(conv[:, :size]) * conv[:, size:]).astype(jnp.bfloat16)


def started(copies):
    for copy in copies:
        copy.start()
    return copies


def gather_rows(pieces, wall, places, chunk):
    for n, piece in enumerate(pieces):
        wall[pl.ds(pl.multiple_of(places[2 + n] * chunk, chunk), chunk), :] = piece[...]


def near_kernel(count, chunk, depth, places, taps, *rest):
    owns, others, pieces = rest[:depth], rest[depth : 2 * depth], rest[2 * depth : 2 * depth + count]
    hidden, left, wall = rest[2 * depth + count :]
    rows, half = owns[0].shape
    gather_rows(pieces, wall, places, chunk)
    for k in range(depth):
        for block, side in ((owns[k], places[0]), (others[k], 1 - places[0])):
            left[rows * k : rows * (k + 1), pl.ds(pl.multiple_of(side * half, 128), half)] = block[...]
    hidden_tiles(left, wall, taps.at[places[1]], hidden)


def down_kernel(count, chunk, blocks, given_to, places, *rest):
    hiddens, pieces = rest[:given_to], rest[given_to : given_to + count]
    outs, (wall, now, sem) = rest[given_to + count : -3], rest[-3:]
    rows, half = outs[0].shape
    for n, piece in enumerate(pieces):
        wall[n] = piece[...]
    core, z, p = places[0], places[1], places[2] % 4
    copies = []
    for k, (which, block) in enumerate(blocks):
        left = hiddens[which][rows * block : rows * (block + 1), :]
        for j, side in enumerate((1 - core, core)):
            n = 2 * k + j
            for low in range(0, half, 256):
                block_at = side * (half // chunk) + low // chunk
                right = jnp.concatenate(
                    [
                        wall[4 * (((block_at + i) // 4) ^ z) + (((block_at + i) % 4) ^ p)]
                        for i in range(256 // chunk)
                    ],
                    axis=1,
                )
                now[n, :, low : low + 256] = jnp.dot(
                    left, right, preferred_element_type=jnp.float32
                ).astype(jnp.bfloat16)
            copies += started([pltpu.make_async_copy(now.at[n], outs[n], sem.at[n])])
    for copy in copies:
        copy.wait()


def mixer_kernel(count, chunk, places, tok_own, tok_other, gains, taps, recur_map, input_map, rate, decay, *rest):
    pieces, (out_own, out_other), (wall, sums_ref, mixed_ref, maps) = (
        rest[:count],
        rest[count : count + 2],
        rest[count + 2 :],
    )
    half = tok_own.shape[1]
    local = rate.shape[1]
    gather_rows(pieces, wall, places, chunk)
    maps[...] = jnp.zeros_like(maps)
    block = maps.shape[1]
    size = recur_map.shape[1]
    for head in range(recur_map.shape[0]):
        group, low = divmod(head * size, block)
        maps[group, low : low + size, low : low + size] = recur_map[head]
        maps[group, low : low + size, block + low : block + low + size] = input_map[head]
    own, other = normed_halves(tok_own[...], tok_other[...], gains, places[0])
    at_own = pl.multiple_of(places[0] * half, 128)
    at_other = pl.multiple_of((1 - places[0]) * half, 128)
    sums_ref[...] = (
        jnp.dot(own, wall[pl.ds(at_own, half), : 2 * local], preferred_element_type=jnp.float32)
        + jnp.dot(other, wall[pl.ds(at_other, half), : 2 * local], preferred_element_type=jnp.float32)
    ).astype(jnp.bfloat16)
    rows = own.shape[0]
    row = lax.broadcasted_iota(jnp.int32, (rows, block), 0) % SEQ_LEN
    for group in range(local // block):
        lanes = slice(block * group, block * (group + 1))
        branch = sums_ref[:, lanes].astype(jnp.float32)
        conv = convolved(branch, taps[:, lanes].astype(jnp.float32), row).astype(jnp.bfloat16)
        gates = jnp.dot(conv, maps[group], preferred_element_type=jnp.float32)
        recur = jax.nn.sigmoid(gates[:, :block])
        inner = jax.nn.sigmoid(gates[:, block:])
        loga = -DECAY_RATE_GAIN * recur * rate[:, lanes] + decay[:, lanes]
        state = jnp.sqrt(minus_expm1(2.0 * loga)) * inner * conv.astype(jnp.float32)
        keep = jnp.exp(loga)
        steps = 1
        while steps < SEQ_LEN:
            state = keep * earlier(state, steps, row) + state
            if 2 * steps < SEQ_LEN:
                keep = keep * jnp.where(row >= steps, pltpu.roll(keep, steps, 0), 1.0)
            steps *= 2
        gate = sums_ref[:, local + block * group : local + block * (group + 1)].astype(jnp.float32)
        mixed_ref[:, lanes] = (state * jax.nn.gelu(gate)).astype(jnp.bfloat16)
    mixed = mixed_ref[...]
    for out, at in ((out_own, at_own), (out_other, at_other)):
        out[...] = lax.dot_general(
            mixed, wall[pl.ds(at, half), 2 * local :], NT, preferred_element_type=jnp.float32
        ).astype(jnp.bfloat16)


def split_layer(depth, *arrays):
    return split_layer_body(depth, *arrays)


def split_layer_body(
    depth,
    tokens,
    mixer_norm_gain,
    recurrence_branch_weight,
    output_gate_projection,
    recurrence_conv_taps,
    recurrence_gate_map,
    input_gate_map,
    channel_decay_rate,
    position_log_decay,
    mixer_output_weight,
    feedforward_norm_gain,
    gate_up_weight,
    value_up_weight,
    gate_conv_taps,
    value_conv_taps,
    down_projection_weight,
):
    rows, half = tokens.shape
    local = recurrence_branch_weight.shape[1]
    chunk = recurrence_branch_weight.shape[0]
    units = gate_up_weight.shape[1] // depth
    z, p, c = lax.axis_index("z"), lax.axis_index("p"), lax.axis_index("c")
    swap = [(0, 1), (1, 0)]
    places = jnp.stack(
        [c, z] + [(z ^ s) * 4 + (p ^ m) for s in range(depth) for m in range(4)]
    ).astype(jnp.int32)
    both_taps = jnp.stack(
        [
            jnp.concatenate(
                [
                    taps[:, units * k + low : units * k + low + size]
                    for low, size in tiles(units)
                    for taps in (gate_conv_taps, value_conv_taps)
                ],
                axis=1,
            )
            for k in range(depth)
        ]
    )

    def swapped(values):
        return lax.ppermute(values, "c", swap)

    tokens_other = swapped(tokens)

    mixer_piece = jnp.concatenate(
        [recurrence_branch_weight, output_gate_projection, mixer_output_weight.T], axis=1
    )
    mixer_parts = line_gather(mixer_piece, depth)
    mixer_parts[-1], places_used, both_taps = lax.optimization_barrier((mixer_parts[-1], places, both_taps))
    mixer_pieces = square_gather(mixer_parts)

    shares = pl.pallas_call(
        functools.partial(pack_kernel, depth),
        out_shape=(jax.ShapeDtypeStruct((chunk, 2 * units), jnp.bfloat16),) * depth
        + (jax.ShapeDtypeStruct((units, chunk), jnp.bfloat16),) * depth,
        in_specs=[SMEM, VMEM, VMEM, VMEM],
        out_specs=(ANY,) * (2 * depth),
        scratch_shapes=[
            pltpu.VMEM((depth, chunk, 2 * units), jnp.bfloat16),
            pltpu.SemaphoreType.DMA((2 * depth,)),
        ],
        compiler_params=pltpu.CompilerParams(vmem_limit_bytes=SMALL),
        name="pack",
    )(places, gate_up_weight, value_up_weight, down_projection_weight)
    up_parts = [shares[s] if s == 0 else traded(shares[s], "z", depth, s) for s in range(depth)]
    down_parts = [shares[depth + s] if s == 0 else traded(shares[depth + s], "z", depth, s) for s in range(depth)]
    up_pieces = square_gather(up_parts)
    down_pieces = square_gather(down_parts)

    mine = jax.ShapeDtypeStruct((rows, half), jnp.bfloat16)
    mine_own, mine_other = pl.pallas_call(
        functools.partial(mixer_kernel, len(mixer_pieces), chunk),
        out_shape=(mine, mine),
        in_specs=[SMEM] + [VMEM] * (8 + len(mixer_pieces)),
        out_specs=(VMEM, VMEM),
        scratch_shapes=[
            pltpu.VMEM((2 * half, 3 * local), jnp.bfloat16),
            pltpu.VMEM((rows, 2 * local), jnp.bfloat16),
            pltpu.VMEM((rows, local), jnp.bfloat16),
            pltpu.VMEM((local // 256, 256, 512), jnp.bfloat16),
        ],
        compiler_params=pltpu.CompilerParams(vmem_limit_bytes=SMALL),
        name="mixer",
    )(
        places_used,
        tokens,
        tokens_other,
        mixer_norm_gain.reshape(2, 1, half),
        recurrence_conv_taps,
        recurrence_gate_map,
        input_gate_map,
        channel_decay_rate[None, :],
        position_log_decay,
        *mixer_pieces,
    )
    theirs_own, theirs_other = swapped(mine_other), swapped(mine_own)

    after_own, normed_own, normed_other = pl.pallas_call(
        join_kernel,
        out_shape=(mine,) * 3,
        in_specs=[SMEM] + [VMEM] * 7,
        out_specs=(VMEM,) * 3,
        compiler_params=pltpu.CompilerParams(vmem_limit_bytes=SMALL),
        name="join",
    )(
        places_used,
        tokens,
        tokens_other,
        mine_own,
        mine_other,
        theirs_own,
        theirs_other,
        feedforward_norm_gain.reshape(2, 1, half),
    )
    owns = line_gather(normed_own, depth)
    others = [normed_other] + [swapped(owns[s]) for s in range(1, depth)]

    count = len(up_pieces)

    def up(members):
        size = len(members)
        return pl.pallas_call(
            functools.partial(near_kernel, count, chunk, size),
            out_shape=jax.ShapeDtypeStruct((size * rows, units), jnp.bfloat16),
            in_specs=[SMEM] + [VMEM] * (1 + 2 * size + count),
            out_specs=VMEM,
            scratch_shapes=[
                pltpu.VMEM((size * rows, 2 * half), jnp.bfloat16),
                pltpu.VMEM((2 * half, 2 * units), jnp.bfloat16),
            ],
            compiler_params=pltpu.CompilerParams(vmem_limit_bytes=SMALL),
        )(places_used, both_taps, *[owns[s] for s in members], *[others[s] for s in members], *up_pieces)

    def down(hidden, members):
        hiddens = [hidden]
        blocks = [(0, s % (depth // 2)) for s in members]
        outs = pl.pallas_call(
            functools.partial(down_kernel, count, chunk, blocks, len(hiddens)),
            out_shape=(mine,) * (2 * len(members)),
            in_specs=[SMEM] + [VMEM] * (len(hiddens) + count),
            out_specs=(ANY,) * (2 * len(members)),
            scratch_shapes=[
                pltpu.VMEM((count, units, chunk), jnp.bfloat16),
                pltpu.VMEM((2 * len(members), rows, half), jnp.bfloat16),
                pltpu.SemaphoreType.DMA((2 * len(members),)),
            ],
            compiler_params=pltpu.CompilerParams(vmem_limit_bytes=SMALL),
        )(places_used, *hiddens, *down_pieces)
        return {s: (outs[2 * k + 1], outs[2 * k]) for k, s in enumerate(members)}

    hidden = up(list(range(depth // 2)))
    hidden_late = up(list(range(depth // 2, depth)))
    products = down(hidden_late, [*range(depth - 1, depth // 2 - 1, -1)])
    products |= down(hidden, [*range(depth // 2 - 1, -1, -1)])
    blocks = []
    for s in range(depth):
        kept, given = products[s]
        taken = swapped(given)
        block = kept.astype(jnp.float32) + taken.astype(jnp.float32)
        blocks.append(block if s == 0 else block.astype(jnp.bfloat16))
    total = line_scatter(blocks, depth)
    return (after_own.astype(jnp.float32) + total).astype(jnp.bfloat16)


def solution(mesh):
    placed = (
        P("fs", "tp"),
        P(),
        P("fs", "tp"),
        P("fs", "tp"),
        P(None, "tp"),
        P("tp", None, None),
        P("tp", None, None),
        P("tp"),
        P("fs", "tp"),
        P("tp", "fs"),
        P(),
        P("fs", "tp"),
        P("fs", "tp"),
        P(None, "tp"),
        P(None, "tp"),
        P("tp", "fs"),
    )
    shards, cores = mesh.shape["fs"], mesh.shape["tp"]
    if cores != 2 or shards not in (8, 16):
        return jax.shard_map(
            gathered_layer, mesh=mesh, in_specs=placed, out_specs=P("fs", "tp"), check_vma=False
        )
    depth = shards // 4
    finer = Mesh(mesh.devices.reshape(depth, 4, cores), ("z", "p", "c"))
    names = {"fs": ("z", "p"), "tp": "c", None: None}
    split = tuple(P(*[names[name] for name in spec]) for spec in placed)
    return jax.shard_map(
        functools.partial(split_layer, depth),
        mesh=finer,
        in_specs=split,
        out_specs=P(("z", "p"), "c"),
        check_vma=False,
    )
```
